256 devices in a mesh: sp: 32 (over z, y), tp: 8 (over x, core).
Axes of the slice: x: 4, y: 4, z: 8, core: 2. Of those that a mesh axis runs over, the one named last changes fastest.
Arguments:
- inputs: bfloat16 [16384, 2048], P('sp', 'tp'), may hold values from -6 to 6
- norm_gain: float32 [2048], replicated, may hold values from 0.1 to 1.9
- latent_query: bfloat16 [2048, 1536], P(None, 'tp'), may hold values from -2 to 2
- latent_down: bfloat16 [2048, 512], replicated, may hold values from -2 to 2
- rope_down: bfloat16 [2048, 32], replicated, may hold values from -2 to 2
- latent_gain: float32 [512], replicated, may hold values from 0.1 to 1.9
- latent_up: bfloat16 [512, 2048], P(None, 'tp'), may hold values from -2 to 2
- window_query: bfloat16 [2048, 1024], P(None, 'tp'), may hold values from -2 to 2
- window_key: bfloat16 [2048, 512], P(None, 'tp'), may hold values from -2 to 2
- window_value: bfloat16 [2048, 512], P(None, 'tp'), may hold values from -0.125 to 0.125
- sink_logit: float32 [16], P('tp'), may hold values from 3 to 8
- out_latent: bfloat16 [1024, 2048], P('tp'), may hold values from -0.1875 to 0.1875
- out_window: bfloat16 [1024, 2048], P('tp'), may hold values from -0.1875 to 0.1875
Outputs:
- attended: bfloat16 [16384, 2048], P('sp', 'tp')
The draws below stay inside these ranges and needn't reach their ends.
All inputs are finite; a program needn't handle non-finite values.
Results may differ from the reference program's by a relative error of at most 0.017.
Values may be sent and summed in bfloat16 or wider, within the bound.
No kernel may reach another device: no remote copies, remote signals or barrier semaphores. Data moves between devices by JAX's collectives and lax.ppermute only.
A program may use at most 128 MiB of HBM per device.

```python
import jax
import jax.numpy as jnp
from jax import lax

D = 2048
HM = 16
HS = 16
HK = 8
LATENT = 512
NOPE = 64
ROPE = 32
HEAD = 64
WINDOW = 128
TOKENS = 16384
N_TP = 8


def latent_tables(key):
    streams = jax.random.split(jax.random.fold_in(key, 7001), 5)
    lowering = jax.random.normal(streams[0], (D, LATENT), jnp.float32) * D ** (-0.5)
    rotating = jax.random.normal(streams[1], (D, ROPE), jnp.float32) * D ** (-0.5)
    raising = jax.random.normal(streams[2], (LATENT, HM * (NOPE + HEAD)), jnp.float32) * LATENT ** (-0.5)
    queries = jax.random.normal(streams[4], (D, HM * (NOPE + ROPE)), jnp.float32) * 2.5 * D ** (-0.5)
    return (jnp.clip(queries, -2.0, 2.0), jnp.clip(lowering, -2.0, 2.0), jnp.clip(rotating, -2.0, 2.0), jnp.clip(raising, -2.0, 2.0))


def window_tables(key):
    streams = jax.random.split(jax.random.fold_in(key, 7002), 3)
    key_weights = jax.random.normal(streams[0], (D, HK * HEAD), jnp.float32) * D ** (-0.5)
    queries = jax.random.normal(streams[2], (D, HS * HEAD), jnp.float32) * 2.0 * D ** (-0.5)
    return (jnp.clip(queries, -2.0, 2.0), jnp.clip(key_weights, -2.0, 2.0))


def draw_latent_query(key, part):
    return latent_tables(key)[0].astype(jnp.bfloat16)


def draw_latent_down(key, part):
    return latent_tables(key)[1].astype(jnp.bfloat16)


def draw_rope_down(key, part):
    return latent_tables(key)[2].astype(jnp.bfloat16)


def draw_latent_up(key, part):
    return latent_tables(key)[3].astype(jnp.bfloat16)


def draw_window_query(key, part):
    return window_tables(key)[0].astype(jnp.bfloat16)


def draw_window_key(key, part):
    return window_tables(key)[1].astype(jnp.bfloat16)


def level_of(key, dims, pieces, smallest, top_value):
    def one(dim, blocks):
        steps = jax.random.uniform(jax.random.fold_in(jax.random.fold_in(key, 6), dim), (blocks,), jnp.float32, smallest / len(pieces), top_value / len(pieces))
        return jnp.repeat(jnp.exp(steps), dims[dim] // blocks).reshape((-1,) + (1,) * (len(dims) - dim - 1))

    level = one(*pieces[0])
    for cut in pieces[1:]:
        level = level * one(*cut)
    return level


def centred(stream_key, dims, width, most, cuts=(), kind=jnp.bfloat16):
    values = jax.random.normal(stream_key, dims, jnp.float32) * width
    if len(cuts) > 0:
        values = level_of(stream_key, dims, cuts, -0.22, 0.18) * values
    return jnp.clip(values, min=-most, max=most).astype(kind)


def setup_inputs(seed: int = 0) -> dict:
    splits = jax.random.split(jax.random.key(seed), 14)
    return {
        "inputs": centred(splits[0], (TOKENS, D), 1.0, 6.0, ((0, 32), (1, 8))),
        "norm_gain": jnp.clip(1.0 + 0.18 * jax.random.normal(splits[1], (D,), jnp.float32), 0.1, 1.9),
        "latent_query": draw_latent_query(jax.random.fold_in(splits[13], 71), 0),
        "latent_down": draw_latent_down(jax.random.fold_in(splits[13], 71), 0),
        "rope_down": draw_rope_down(jax.random.fold_in(splits[13], 71), 0),
        "latent_gain": jnp.clip(1.0 + 0.18 * jax.random.normal(splits[5], (LATENT,), jnp.float32), 0.1, 1.9),
        "latent_up": draw_latent_up(jax.random.fold_in(splits[13], 71), 0),
        "window_query": draw_window_query(jax.random.fold_in(splits[13], 71), 0),
        "window_key": draw_window_key(jax.random.fold_in(splits[13], 71), 0),
        "window_value": centred(splits[9], (D, HK * HEAD), D ** -0.5, 0.125, ((1, 8),)),
        "sink_logit": jnp.clip(3.0 + 5.0 * jax.random.uniform(splits[10], (HS,), jnp.float32) ** level_of(splits[10], (HS,), ((0, 8),), -0.2, 0.2), 3.0, 8.0),
        "out_latent": centred(splits[11], (HM * HEAD, D), (HM * HEAD) ** -0.5, 0.1875, ((0, 8),)),
        "out_window": centred(splits[12], (HS * HEAD, D), (HS * HEAD) ** -0.5, 0.1875, ((0, 8),)),
    }


epsilon = 1e-06

def rms_scale(values, gains):
    return values * lax.rsqrt(lax.optimization_barrier(jnp.mean(values * values, axis=-1, keepdims=True)) + epsilon) * gains

def rotary(values, positions):
    half_width = values.shape[-1] // 2
    inverse = 1.0 / 10000.0 ** (jnp.arange(0, 2 * half_width, 2).astype(jnp.float32) / (2 * half_width))
    angles = positions[:, None] * inverse[None, :]
    cosine_table = jnp.cos(angles)[:, None, :]
    sine_table = jnp.sin(angles)[:, None, :]
    first_half = values[..., :half_width]
    second_half = values[..., half_width:]
    return jnp.concatenate([first_half * cosine_table - second_half * sine_table, second_half * cosine_table + first_half * sine_table], axis=-1)

def reference(inputs, norm_gain, latent_query, latent_down, rope_down, latent_gain, latent_up, window_query, window_key, window_value, sink_logit, out_latent, out_window):
    length_all = inputs.shape[0]
    positions = jnp.arange(length_all).astype(jnp.float32)
    hidden = rms_scale(inputs.astype(jnp.float32), norm_gain).astype(jnp.bfloat16)
    latent = rms_scale(jnp.dot(hidden, latent_down, preferred_element_type=jnp.float32), latent_gain).astype(jnp.bfloat16)
    shared = rotary(jnp.dot(hidden, rope_down, preferred_element_type=jnp.float32)[:, None, :], positions)[:, 0, :].astype(jnp.bfloat16)
    expanded = jnp.dot(latent, latent_up, preferred_element_type=jnp.float32).astype(jnp.bfloat16)
    expanded = expanded.reshape(length_all, HM, NOPE + HEAD)
    queries = jnp.dot(hidden, latent_query, preferred_element_type=jnp.float32).reshape(length_all, HM, NOPE + ROPE)
    queries = jnp.concatenate([queries[..., :NOPE], rotary(queries[..., NOPE:], positions)], axis=-1).astype(jnp.bfloat16)
    key_plain = expanded[..., :NOPE].astype(jnp.float32)
    value_rows = expanded[..., NOPE:].astype(jnp.float32)
    shared_rows = shared.astype(jnp.float32)
    score_scale = (NOPE + ROPE) ** (-0.5)

    def latent_block(query_block):
        query_block = query_block.astype(jnp.float32)
        scores = (jnp.einsum('qhn,khn->hqk', query_block[..., :NOPE], key_plain) + jnp.einsum('qhr,kr->hqk', query_block[..., NOPE:], shared_rows)) * score_scale
        highest = lax.optimization_barrier(jnp.max(scores, axis=-1, keepdims=True))
        weights = jnp.exp(scores - highest)
        summed = lax.optimization_barrier(jnp.sum(weights, axis=-1))
        rounded = lax.optimization_barrier(weights.astype(jnp.bfloat16)).astype(jnp.float32)
        mixture = jnp.einsum('hqk,khd->qhd', rounded, value_rows)
        return mixture / jnp.transpose(summed)[:, :, None]
    query_blocks = queries.reshape(length_all // WINDOW, WINDOW, HM, NOPE + ROPE)
    latent_out = lax.map(latent_block, query_blocks).reshape(length_all, HM * HEAD).astype(jnp.bfloat16)
    group_size = HS // HK
    block_count = length_all // WINDOW
    window_queries = rotary(jnp.dot(hidden, window_query, preferred_element_type=jnp.float32).reshape(length_all, HS, HEAD), positions).astype(jnp.bfloat16)
    window_keys = rotary(jnp.dot(hidden, window_key, preferred_element_type=jnp.float32).reshape(length_all, HK, HEAD), positions).astype(jnp.bfloat16)
    window_values = jnp.dot(hidden, window_value, preferred_element_type=jnp.float32).astype(jnp.bfloat16).reshape(length_all, HK, HEAD)

    def banded(values):
        padded = jnp.pad(values, ((WINDOW, WINDOW), (0, 0), (0, 0)))
        grid_rows = padded.reshape(block_count + 2, WINDOW, HK, HEAD)
        return jnp.concatenate([grid_rows[:-2], grid_rows[1:-1], grid_rows[2:]], axis=1)
    band_keys = banded(window_keys).astype(jnp.float32)
    band_values = banded(window_values).astype(jnp.float32)
    query_band = window_queries.reshape(block_count, WINDOW, HK, group_size, HEAD).astype(jnp.float32)
    offsets = jnp.arange(3 * WINDOW)[None, :] - jnp.arange(WINDOW)[:, None]
    key_pos = jnp.arange(block_count)[:, None] * WINDOW - WINDOW + jnp.arange(3 * WINDOW)[None, :]
    allowed = ((offsets >= 0) & (offsets <= 2 * WINDOW))[None] & ((key_pos >= 0) & (key_pos < length_all))[:, None, :]
    sink_table = sink_logit.reshape(HK, group_size)

    def window_head(operands):
        head_queries, head_keys, head_values, head_sinks = operands
        scores = jnp.einsum('nqgd,nkd->ngqk', head_queries, head_keys) * HEAD ** (-0.5)
        scores = jnp.where(allowed[:, None], scores, -jnp.inf)
        highest = jnp.maximum(lax.optimization_barrier(jnp.max(scores, axis=-1)), head_sinks[None, :, None])
        weights = jnp.exp(scores - highest[..., None])
        summed = lax.optimization_barrier(jnp.sum(weights, axis=-1)) + jnp.exp(head_sinks[None, :, None] - highest)
        rounded = lax.optimization_barrier(weights.astype(jnp.bfloat16)).astype(jnp.float32)
        mixture = jnp.einsum('ngqk,nkd->nqgd', rounded, head_values)
        return mixture / jnp.transpose(summed, (0, 2, 1))[..., None]
    stacked = lax.map(window_head, (jnp.moveaxis(query_band, 2, 0), jnp.moveaxis(band_keys, 2, 0), jnp.moveaxis(band_values, 2, 0), sink_table))
    window_out = jnp.moveaxis(stacked, 0, 2).reshape(length_all, HS * HEAD).astype(jnp.bfloat16)
    latent_cols = HM * HEAD // N_TP
    window_cols = HS * HEAD // N_TP
    result = jnp.zeros((length_all, D), jnp.float32)
    for group_index in range(N_TP):
        partial_value = jnp.dot(latent_out[:, group_index * latent_cols:(group_index + 1) * latent_cols], out_latent[group_index * latent_cols:(group_index + 1) * latent_cols], preferred_element_type=jnp.float32)
        partial_value = partial_value + jnp.dot(window_out[:, group_index * window_cols:(group_index + 1) * window_cols], out_window[group_index * window_cols:(group_index + 1) * window_cols], preferred_element_type=jnp.float32)
        result = result + lax.optimization_barrier(partial_value.astype(jnp.bfloat16)).astype(jnp.float32)
    return result.astype(jnp.bfloat16)
```

```python
import functools
import math

import jax
import jax.numpy as jnp
import numpy as np
from jax import lax
from jax.experimental import pallas as pl
from jax.experimental.pallas import tpu as pltpu
from jax.sharding import Mesh
from jax.sharding import PartitionSpec as P


NOPE = 64
ROPE = 32
HEAD = 64
WINDOW = 128
TILE = 256
epsilon = 1e-06
LOG2E = math.log2(math.e)
LATENT_SCALE = LOG2E * (NOPE + ROPE) ** (-0.5)
WINDOW_SCALE = LOG2E * HEAD ** (-0.5)
GRANT = 12 << 20
SMALLEST = 2.0**-60
LARGEST = 2.0**100
F32 = jnp.float32
BF16 = jnp.bfloat16
VMEM = pltpu.VMEM


NT = (((1,), (1,)), ((), ()))


def dot(a, b):
    return jnp.dot(a, b, preferred_element_type=F32)


def dot_nt(a, b):
    return lax.dot_general(a, b, NT, preferred_element_type=F32)


def rotate(v, cos, sin):
    half = v.shape[0] // 2
    a, b = v[:half], v[half:]
    return jnp.concatenate([a * cos - b * sin, b * cos + a * sin], axis=0)


def params(grant=GRANT):
    return pltpu.CompilerParams(vmem_limit_bytes=grant)


def vmem(count):
    return [pl.BlockSpec(memory_space=VMEM)] * count


SMEM = pl.BlockSpec(memory_space=pltpu.SMEM)
HBM = pl.BlockSpec(memory_space=pltpu.HBM)
ANY = pl.BlockSpec(memory_space=pl.ANY)


def stage_kernel(lq_hbm, rope_hbm, wk_hbm, wv_hbm, wq_hbm, up_hbm, rows_ref, up_out, wq_ref, up_ref, sems):
    copies = [
        pltpu.make_async_copy(wq_hbm, wq_ref, sems.at[0]),
        pltpu.make_async_copy(up_hbm, up_ref, sems.at[1]),
        pltpu.make_async_copy(lq_hbm, rows_ref.at[0:192], sems.at[2]),
        pltpu.make_async_copy(rope_hbm, rows_ref.at[192:224], sems.at[3]),
        pltpu.make_async_copy(wk_hbm, rows_ref.at[224:288], sems.at[4]),
        pltpu.make_async_copy(wv_hbm, rows_ref.at[288:352], sems.at[5]),
    ]
    for copy in copies:
        copy.start()
    copies[0].wait()
    rows_ref[352:480] = wq_ref[...].T
    copies[1].wait()
    up_out[...] = up_ref[...].T
    for copy in copies[2:]:
        copy.wait()


def stage(*weights):
    return pl.pallas_call(
        stage_kernel,
        out_shape=[
            jax.ShapeDtypeStruct((480, 2048), BF16),
            jax.ShapeDtypeStruct((256, 512), BF16),
        ],
        in_specs=[HBM] * len(weights),
        out_specs=vmem(2),
        scratch_shapes=[
            VMEM((2048, 128), BF16),
            VMEM((512, 256), BF16),
            pltpu.SemaphoreType.DMA((6,)),
        ],
        compiler_params=params(),
        cost_estimate=pl.CostEstimate(flops=1 << 30, bytes_accessed=9 << 20, transcendentals=0),
        name="stage",
    )(*weights)


def project_kernel(
    place,
    x_refs,
    gain_ref,
    lgain_ref,
    rows_ref,
    up_ref,
    cos_ref,
    sin_ref,
    down_hbm,
    chunk_refs,
    wq_out,
    wkv_out,
    hid,
    down_ref,
    sem,
):
    chip, line, core = place[0], place[1], place[2]
    blocks = gain_ref.shape[0]
    width = gain_ref.shape[2]
    fetch = pltpu.make_async_copy(down_hbm, down_ref, sem)
    fetch.start()
    for part in range(2):
        at = slice(part * TILE, (part + 1) * TILE)
        pieces = []
        for ref, chips, cores, rows in x_refs:
            if rows is None:
                pieces.append((ref, at, chips, cores))
            elif rows == part:
                pieces.append((ref, slice(0, TILE), chips, cores))
        total = jnp.zeros((TILE, 1), F32)
        for ref, rows, _, _ in pieces:
            x = ref[rows].astype(F32)
            total += jnp.sum(x * x, axis=1, keepdims=True)
        scale = lax.rsqrt(total / (blocks * width) + epsilon)
        for ref, rows, chips, cores in pieces:
            block = 2 * ((chip + chips) % 4) + (core + cores) % 2
            x = ref[rows].astype(F32)
            hid[part, :, pl.ds(pl.multiple_of(block * width, width), width)] = (
                x * scale * gain_ref[block]
            ).astype(BF16)
    fetch.wait()
    for part in range(2):
        at = slice(part * TILE, (part + 1) * TILE)
        hidden = hid[part]
        cos64, sin64 = cos_ref[0:32, at], sin_ref[0:32, at]
        cos32, sin32 = cos_ref[32:48, at], sin_ref[32:48, at]
        raw = dot(hidden, down_ref[...])
        mean = jnp.mean(raw * raw, axis=1, keepdims=True)
        latent = (raw * lax.rsqrt(mean + epsilon) * lgain_ref[...]).astype(BF16)
        together = dot_nt(rows_ref[...], hidden)
        expanded = dot_nt(up_ref[...], latent).astype(BF16)
        queries = together[0:192]
        shared = rotate(together[192:224], cos32, sin32).astype(BF16)
        for h in range(2):
            base = h * (NOPE + ROPE)
            own = h * (NOPE + HEAD)
            plain = (queries[base : base + NOPE] * LATENT_SCALE).astype(BF16)
            turned = (
                rotate(queries[base + NOPE : base + NOPE + ROPE], cos32, sin32) * LATENT_SCALE
            ).astype(BF16)
            turn = (2 * h + part - line + 4) % 4
            for r, out in enumerate(chunk_refs):

                @pl.when(turn == r)
                def _():
                    out[0:64] = plain
                    out[64:96] = turned
                    out[96:160] = expanded[own : own + NOPE]
                    out[160:192] = shared
                    out[192:256] = expanded[own + NOPE : own + NOPE + HEAD]

        window_q = together[352:480]
        first = (rotate(window_q[0:64], cos64, sin64) * WINDOW_SCALE).astype(BF16)
        second = (rotate(window_q[64:128], cos64, sin64) * WINDOW_SCALE).astype(BF16)
        for n in range(2):
            cut = slice(n * WINDOW, (n + 1) * WINDOW)
            wq_out[2 * part + n, :, 0:WINDOW] = first[:, cut]
            wq_out[2 * part + n, :, WINDOW : 2 * WINDOW] = second[:, cut]
        wkv_out[0:64, at] = rotate(together[224:288], cos64, sin64).astype(BF16)
        wkv_out[64:128, at] = together[288:352].astype(BF16)


def project(place, pieces, weights, rows):
    where = [piece[1:] for piece in pieces]
    arrays = [piece[0] for piece in pieces]
    n = len(arrays)

    def kernel(place_ref, *refs):
        x_refs = [(ref, *at) for ref, at in zip(refs[:n], where)]
        inputs = refs[n : n + len(weights)]
        outs = refs[n + len(weights) :]
        project_kernel(place_ref, x_refs, *inputs, outs[:4], *outs[4:])

    return pl.pallas_call(
        kernel,
        out_shape=[jax.ShapeDtypeStruct((256, TILE), BF16)] * 4
        + [
            jax.ShapeDtypeStruct((rows // WINDOW, 64, 2 * WINDOW), BF16),
            jax.ShapeDtypeStruct((128, rows), BF16),
        ],
        in_specs=[SMEM] + vmem(n + len(weights) - 1) + [HBM],
        out_specs=vmem(6),
        scratch_shapes=[
            VMEM((2, TILE, 2048), BF16),
            VMEM((2048, 512), BF16),
            pltpu.SemaphoreType.DMA(()),
        ],
        compiler_params=params(16 << 20),
        cost_estimate=pl.CostEstimate(
            flops=2 * rows * 2048 * 1024, bytes_accessed=8 << 20, transcendentals=0
        ),
        name="project",
    )(place, *arrays, *weights)


def attend_kernel(first, last, tiles, kv_count, place, *refs):
    q_refs, refs = refs[:tiles], refs[tiles:]
    kv_refs, refs = refs[:kv_count], refs[kv_count:]
    if not first:
        total_in, sum_in, refs = refs[0], refs[1], refs[2:]
    if last:
        all_refs, refs = refs[:-7], refs[-7:]
        out_ref, total, sums, buf, held, everything, sem = refs
    else:
        total, sums, buf, held = refs
    if first:
        total[...] = jnp.zeros_like(total)
        sums[...] = jnp.zeros_like(sums)
    else:
        total[...] = total_in[...]
        sums[...] = sum_in[...]
    inner, _, keys = kv_refs[0].shape
    for n, ref in enumerate(kv_refs):
        held[n * inner : (n + 1) * inner] = ref[...]
    count = kv_count * inner

    def add(t, p, v):
        sums[t] += p.reshape(keys // 8, 8, TILE).sum(axis=0)
        total[t] += dot(v, p.astype(BF16))

    k = held[0, 0:96, :].T
    for t in range(tiles):
        buf[0, t] = dot(k, q_refs[t][0:96])

    def step(i, carry):
        for b in range(2):
            now = 2 * i + b
            k = held[jnp.minimum(now + 1, count - 1), 0:96, :].T
            v = held[now, 96:160, :]
            for t in range(tiles):
                buf[1 - b, t] = dot(k, q_refs[t][0:96])
                add(t, jnp.exp2(buf[b, t]), v)
        return carry

    lax.fori_loop(0, count // 2, step, 0)
    if not last:
        return

    columns = jnp.sum(sums[...], axis=1)
    fits = (jnp.min(columns) >= SMALLEST) & (jnp.max(columns) <= LARGEST)

    @pl.when(jnp.logical_not(fits))
    def _():
        for n, ref in enumerate(all_refs):
            copy = pltpu.make_async_copy(ref, everything.at[n * inner : (n + 1) * inner], sem)
            copy.start()
            copy.wait()
        for t in range(tiles):
            total[t] = jnp.zeros_like(total[t])
            sums[t] = jnp.zeros_like(sums[t])

            def again(b, shift, t=t):
                s = dot(everything[b, 0:96, :].T, q_refs[t][0:96])
                new = jnp.maximum(shift, jnp.max(s, axis=0, keepdims=True))
                shrink = jnp.exp2(shift - new)
                sums[t] *= shrink
                total[t] *= shrink
                add(t, jnp.exp2(s - new), everything[b, 96:160, :])
                return new

            lax.fori_loop(
                0, len(all_refs) * inner, again, jnp.full((1, TILE), -jnp.inf, F32)
            )

    for t in range(tiles):
        line = (place[3] - t + 4) % 4
        out_ref[line] = (total[t] / jnp.sum(sums[t], axis=0, keepdims=True)).astype(BF16)


def attend(place, chunks, kvs, state=None, everything=None):
    tiles = len(chunks)
    first, last = state is None, everything is not None
    inner, depth, keys = kvs[0].shape
    holds = [(tiles, HEAD, TILE), (tiles, 8, TILE)]
    spare = [
        VMEM((2, tiles, keys, TILE), F32),
        VMEM((len(kvs) * inner, depth, keys), BF16),
    ]
    args = (*chunks, *kvs) + (() if first else tuple(state))
    in_specs = [SMEM] + vmem(len(args))
    if last:
        out_shape = [jax.ShapeDtypeStruct((tiles, HEAD, TILE), BF16)]
        spare = [VMEM(s, F32) for s in holds] + spare
        spare += [
            VMEM((len(everything) * inner, depth, keys), BF16),
            pltpu.SemaphoreType.DMA(()),
        ]
        args += tuple(everything)
        in_specs += [ANY] * len(everything)
    else:
        out_shape = [jax.ShapeDtypeStruct(s, F32) for s in holds]
    work = tiles * TILE * len(kvs) * inner * keys
    return pl.pallas_call(
        functools.partial(attend_kernel, first, last, tiles, len(kvs)),
        out_shape=out_shape,
        in_specs=in_specs,
        out_specs=vmem(len(out_shape)),
        scratch_shapes=spare,
        compiler_params=params(),
        cost_estimate=pl.CostEstimate(
            flops=2 * work * 320, bytes_accessed=3 << 20, transcendentals=work
        ),
        name="attend_last" if last else "attend",
    )(place, *args)


def window_kernel(span_ref, q_ref, kv_ref, left_ref, right_ref, sink_ref, out_ref, ext):
    rows = kv_ref.shape[1]
    ext[:, 0:WINDOW] = left_ref[...]
    ext[:, WINDOW : WINDOW + rows] = kv_ref[...]
    ext[:, WINDOW + rows :] = right_ref[...]
    first_span, last_span = span_ref[0] == 0, span_ref[0] == span_ref[1] - 1
    wide = 3 * WINDOW
    key = lax.broadcasted_iota(jnp.int32, (wide, 2 * WINDOW), 0)
    lane = lax.broadcasted_iota(jnp.int32, (wide, 2 * WINDOW), 1)
    offset = key - jnp.where(lane >= WINDOW, lane - WINDOW, lane)
    near = (offset >= 0) & (offset <= 2 * WINDOW)
    side = lax.broadcasted_iota(jnp.int32, (1, 2 * WINDOW), 1)
    sink = jnp.where(side < WINDOW, sink_ref[0], sink_ref[1]) * LOG2E
    blocks = rows // WINDOW
    for n in range(blocks):
        k = ext[0:64, n * WINDOW : n * WINDOW + wide].T
        v = ext[64:128, n * WINDOW : n * WINDOW + wide]
        allowed = near
        if n == 0:
            allowed = allowed & ((key >= WINDOW) | jnp.logical_not(first_span))
        if n == blocks - 1:
            allowed = allowed & ((key < 2 * WINDOW) | jnp.logical_not(last_span))
        s = jnp.where(allowed, dot(k, q_ref[n]), -jnp.inf)
        top = jnp.maximum(jnp.max(s, axis=0, keepdims=True), sink)
        p = jnp.exp2(s - top)
        denom = jnp.sum(p, axis=0, keepdims=True) + jnp.exp2(sink - top)
        o = (dot(v, p.astype(BF16)) / denom).astype(BF16)
        out_ref[0:64, n * WINDOW : (n + 1) * WINDOW] = o[:, 0:WINDOW]
        out_ref[64:128, n * WINDOW : (n + 1) * WINDOW] = o[:, WINDOW:]


def windowed(span, q, kv, left, right, sink):
    smem = pl.BlockSpec(memory_space=pltpu.SMEM)
    vmem = pl.BlockSpec(memory_space=VMEM)
    rows = kv.shape[1]
    return pl.pallas_call(
        window_kernel,
        out_shape=jax.ShapeDtypeStruct((128, rows), BF16),
        in_specs=[smem, vmem, vmem, vmem, vmem, smem],
        out_specs=vmem,
        scratch_shapes=[VMEM((128, rows + 2 * WINDOW), BF16)],
        cost_estimate=pl.CostEstimate(
            flops=rows * 2 * 384 * 256, bytes_accessed=1 << 20, transcendentals=rows * 768
        ),
        compiler_params=params(),
        name="windowed",
    )(span, q, kv, left, right, sink)


def merge_kernel(place, keep_ref, got_ref, win_ref, wl_ref, ww_ref, *refs):
    own_refs, sib_refs, (mixed, lhs) = refs[:4], refs[4:8], refs[8:]
    chip, core = place[0], place[2]
    for ref, half in ((keep_ref, core), (got_ref, 1 - core)):
        at = pl.ds(pl.multiple_of(half * TILE, TILE), TILE)
        mixed[0:HEAD, at] = ref[0]
        mixed[HEAD : 2 * HEAD, at] = ref[1]
    lhs[:, 0:128] = mixed[...].T
    lhs[:, 128:256] = win_ref[...].T
    rows = lhs[...]
    width = own_refs[0].shape[1]
    for outs, side in ((sib_refs, 1 - core), (own_refs, core)):
        for k in (2, 1, 3, 0):
            start = (2 * ((chip + k) % 4) + side) * width
            at = pl.ds(pl.multiple_of(start, width), width)
            both = jnp.concatenate([wl_ref[:, at], ww_ref[:, at]], axis=0)
            outs[k][...] = dot(rows, both).astype(BF16)


def merge(place, keep, got, win, out_latent, out_window):
    rows = win.shape[1]
    return pl.pallas_call(
        merge_kernel,
        out_shape=[jax.ShapeDtypeStruct((rows, 256), BF16)] * 8,
        in_specs=[SMEM] + vmem(5),
        out_specs=vmem(8),
        scratch_shapes=[VMEM((128, rows), BF16), VMEM((rows, 256), BF16)],
        compiler_params=params(),
        cost_estimate=pl.CostEstimate(
            flops=2 * rows * 256 * 2048, bytes_accessed=4 << 20, transcendentals=0
        ),
        name="merge",
    )(place, keep, got, win, out_latent, out_window)


SWAP = [(0, 1), (1, 0)]


def shifted(value, axis, by):
    count = lax.axis_size(axis)
    return lax.ppermute(value, axis, [(i, (i + by) % count) for i in range(count)])


def other_core(value):
    return lax.ppermute(value, "c", SWAP)


def ring_step(value):
    count = lax.axis_size("z")
    up = [(2 * i, 2 * ((i + 1) % count)) for i in range(count)]
    down = [(2 * i + 1, 2 * ((i - 1) % count) + 1) for i in range(count)]
    return lax.ppermute(value, ("z", "c"), up + down)


def head_routes(turn):
    routes = []
    for y in range(4):
        d = (y + turn) % 4
        for c in range(2):
            routes.append((2 * y + c, 2 * (2 * c + d // 2) + d % 2))
    return routes


def shards(
    inputs,
    norm_gain,
    latent_query,
    latent_down,
    rope_down,
    latent_gain,
    latent_up,
    window_query,
    window_key,
    window_value,
    sink_logit,
    out_latent,
    out_window,
):
    rows = inputs.shape[0]
    core = lax.axis_index("c")
    line = lax.axis_index("y")
    span = lax.axis_index(("z", "y"))
    spans = lax.axis_size(("z", "y"))
    slot = 2 * (line % 2) + core
    place = jnp.stack([lax.axis_index("x"), line, core, slot]).astype(jnp.int32)

    before = shifted(inputs, "x", 1)
    after = shifted(inputs, "x", -1)
    far_low = shifted(before[:TILE], "x", 1)
    far_high = shifted(after[TILE:], "x", -1)
    held = [
        (inputs, 0, None),
        (before, 3, None),
        (after, 1, None),
        (far_low, 2, 0),
        (far_high, 2, 1),
    ]
    pieces = []
    for array, chips, part in held:
        pieces.append((array, chips, 0, part))
        pieces.append((other_core(array), chips, 1, part))

    staged = stage(
        latent_query.T,
        rope_down.T,
        window_key.T,
        window_value.T,
        window_query,
        latent_up,
    )
    powers = np.arange(0, HEAD, 2).astype(np.float64) / HEAD
    inverse = 1.0 / 10000.0**powers
    inverse = jnp.asarray(np.concatenate([inverse, inverse[::2]]), F32)
    positions = (span * rows + jnp.arange(rows)).astype(F32)
    angles = inverse[:, None] * positions[None, :]
    tables = jnp.cos(angles), jnp.sin(angles)
    *chunks, wq, wkv = project(
        place,
        pieces,
        (norm_gain.reshape(8, 1, 256), latent_gain[None], *staged, *tables, latent_down),
        rows,
    )
    mine = [lax.ppermute(c, ("y", "c"), head_routes(r)) for r, c in enumerate(chunks)]
    left = lax.ppermute(
        wkv[:, rows - WINDOW :], ("z", "y"), [(i, i + 1) for i in range(spans - 1)]
    )
    right = lax.ppermute(
        wkv[:, :WINDOW], ("z", "y"), [(i + 1, i) for i in range(spans - 1)]
    )
    where = jnp.stack([span, spans]).astype(jnp.int32)
    win = windowed(where, wq, wkv, left, right, sink_logit)

    low = jnp.stack([c[96:256] for c in mine])
    high = other_core(low)
    state = None
    seen = []
    for n in range(4):
        ring_low, ring_high = low, high
        low = ring_step(low)
        if n < 3:
            high = ring_step(high)
        blocks = [ring_low, ring_high]
        if n:
            blocks += [other_core(ring_low), other_core(ring_high)]
        state = attend(place, mine, blocks, state)
        seen += blocks
    blocks = [low, other_core(low)]
    (mixed,) = attend(place, mine, blocks, state, seen + blocks)

    back = lax.all_to_all(mixed, "y", 0, 0, tiled=True)
    pairs = back.reshape(2, 2, HEAD, TILE)
    keep = lax.dynamic_index_in_dim(pairs, core, 0, keepdims=False)
    give = lax.dynamic_index_in_dim(pairs, 1 - core, 0, keepdims=False)
    sums = merge(place, keep, other_core(give), win, out_latent, out_window)
    total = 0
    for k in (2, 1, 3, 0):
        own, sibling = sums[k], other_core(sums[4 + k])
        both = own.astype(F32) + sibling.astype(F32)
        if k:
            both = shifted(both.astype(BF16), "x", k).astype(F32)
        total = total + both
    return total.astype(BF16)


def solution(mesh):
    shape = (8, 4, 4, 2)
    torus = Mesh(mesh.devices.reshape(shape), ("z", "y", "x", "c"))
    sp, tp = ("z", "y"), ("x", "c")
    in_specs = (
        P(sp, tp),
        P(),
        P(None, tp),
        P(),
        P(),
        P(),
        P(None, tp),
        P(None, tp),
        P(None, tp),
        P(None, tp),
        P(tp),
        P(tp, None),
        P(tp, None),
    )
    return jax.shard_map(
        shards, mesh=torus, in_specs=in_specs, out_specs=P(sp, tp), check_vma=False
    )
```

```python
import functools
import math

import jax
import jax.numpy as jnp
import numpy as np
from jax import lax
from jax.experimental import pallas as pl
from jax.experimental.pallas import tpu as pltpu
from jax.sharding import Mesh
from jax.sharding import PartitionSpec as P


NOPE = 64
ROPE = 32
HEAD = 64
WINDOW = 128
TILE = 256
epsilon = 1e-06
LOG2E = math.log2(math.e)
LATENT_SCALE = LOG2E * (NOPE + ROPE) ** (-0.5)
WINDOW_SCALE = LOG2E * HEAD ** (-0.5)
GRANT = 12 << 20
PROJECT_GRANT = 60 << 20
SMALLEST = 2.0**-60
LARGEST = 2.0**100
F32 = jnp.float32
BF16 = jnp.bfloat16
VMEM = pltpu.VMEM


NT = (((1,), (1,)), ((), ()))


def dot(a, b):
    return jnp.dot(a, b, preferred_element_type=F32)


def dot_nt(a, b):
    return lax.dot_general(a, b, NT, preferred_element_type=F32)


def rotate(v, cos, sin):
    half = v.shape[0] // 2
    a, b = v[:half], v[half:]
    return jnp.concatenate([a * cos - b * sin, b * cos + a * sin], axis=0)


def params(grant=GRANT):
    return pltpu.CompilerParams(vmem_limit_bytes=grant)


def vmem(count):
    return [pl.BlockSpec(memory_space=VMEM)] * count


SMEM = pl.BlockSpec(memory_space=pltpu.SMEM)
HBM = pl.BlockSpec(memory_space=pltpu.HBM)
ANY = pl.BlockSpec(memory_space=pl.ANY)


def project_kernel(place, gain_ref, lgain_ref, cos_ref, sin_ref, *refs):
    x_hbm, (lq_hbm, rope_hbm, wk_hbm, wv_hbm, wq_hbm, up_hbm, down_hbm), refs = (
        refs[:10],
        refs[10:17],
        refs[17:],
    )
    chunk_refs, (wq_out, wkv_out), refs = refs[:4], refs[4:6], refs[6:]
    xs, hid, rows_ref, wq_ref, up_ref, up_rows, down_ref, sems = refs
    chip, line, core = place[0], place[1], place[2]
    blocks, _, width = xs.shape
    targets = [xs.at[n] for n in range(6)]
    for n in (6, 7):
        targets.insert(len(targets), xs.at[n, 0:TILE])
    for n in (6, 7):
        targets.insert(len(targets), xs.at[n, TILE : 2 * TILE])
    targets += [
        rows_ref.at[0:192],
        rows_ref.at[192:224],
        rows_ref.at[224:288],
        rows_ref.at[288:352],
        wq_ref,
        up_ref,
        down_ref,
    ]
    sources = [*x_hbm, lq_hbm, rope_hbm, wk_hbm, wv_hbm, wq_hbm, up_hbm, down_hbm]
    copies = [
        pltpu.make_async_copy(a, b, sems.at[n]) for n, (a, b) in enumerate(zip(sources, targets))
    ]
    for copy in copies:
        copy.start()
    for copy in copies[:10]:
        copy.wait()

    def normalize(part, carry):
        at = pl.ds(pl.multiple_of(part * TILE, TILE), TILE)
        total = jnp.zeros((TILE, 1), F32)
        for n in range(blocks):
            x = xs[n, at].astype(F32)
            total += jnp.sum(x * x, axis=1, keepdims=True)
        scale = lax.rsqrt(total / (blocks * width) + epsilon)
        for n in range(blocks):
            block = 2 * ((chip + (0, 3, 1, 2)[n // 2]) % 4) + (core + n) % 2
            x = xs[n, at].astype(F32)
            hid[part, :, pl.ds(pl.multiple_of(block * width, width), width)] = (
                x * scale * gain_ref[block]
            ).astype(BF16)
        return carry

    lax.fori_loop(0, 2, normalize, 0)
    for copy in copies[10:]:
        copy.wait()
    rows_ref[352:480] = wq_ref[...].T
    up_rows[...] = up_ref[...].T

    def heads(part, carry):
        at = pl.ds(pl.multiple_of(part * TILE, TILE), TILE)
        hidden = hid[part]
        cos64, sin64 = cos_ref[0:32, at], sin_ref[0:32, at]
        cos32, sin32 = cos_ref[32:48, at], sin_ref[32:48, at]
        raw = dot(hidden, down_ref[...])
        mean = jnp.mean(raw * raw, axis=1, keepdims=True)
        latent = (raw * lax.rsqrt(mean + epsilon) * lgain_ref[...]).astype(BF16)
        together = dot_nt(rows_ref[...], hidden)
        expanded = dot_nt(up_rows[...], latent).astype(BF16)
        queries = together[0:192]
        shared = rotate(together[192:224], cos32, sin32).astype(BF16)
        for h in range(2):
            base = h * (NOPE + ROPE)
            own = h * (NOPE + HEAD)
            plain = queries[base : base + NOPE].astype(BF16)
            turned = rotate(queries[base + NOPE : base + NOPE + ROPE], cos32, sin32).astype(BF16)
            turn = (2 * h + part - line + 4) % 4
            for r, out in enumerate(chunk_refs):

                @pl.when(turn == r)
                def _():
                    out[0:64] = plain
                    out[64:96] = turned
                    out[96:160] = expanded[own : own + NOPE]
                    out[160:192] = shared
                    out[192:256] = expanded[own + NOPE : own + NOPE + HEAD]

        window_q = together[352:480]
        first = rotate(window_q[0:64], cos64, sin64).astype(BF16)
        second = rotate(window_q[64:128], cos64, sin64).astype(BF16)
        for n in range(2):
            cut = slice(n * WINDOW, (n + 1) * WINDOW)
            wq_out[2 * part + n, :, 0:WINDOW] = first[:, cut]
            wq_out[2 * part + n, :, WINDOW : 2 * WINDOW] = second[:, cut]
        wkv_out[0:64, at] = rotate(together[224:288], cos64, sin64).astype(BF16)
        wkv_out[64:128, at] = together[288:352].astype(BF16)
        return carry

    lax.fori_loop(0, 2, heads, 0)


def project(place, small, pieces, weights, rows):
    return pl.pallas_call(
        project_kernel,
        out_shape=[jax.ShapeDtypeStruct((256, TILE), BF16)] * 4
        + [
            jax.ShapeDtypeStruct((rows // WINDOW, 64, 2 * WINDOW), BF16),
            jax.ShapeDtypeStruct((128, rows), BF16),
        ],
        in_specs=[SMEM] + vmem(len(small)) + [HBM] * (len(pieces) + len(weights)),
        out_specs=vmem(6),
        scratch_shapes=[
            VMEM((8, rows, 256), BF16),
            VMEM((2, TILE, 2048), BF16),
            VMEM((480, 2048), BF16),
            VMEM((2048, 128), BF16),
            VMEM((512, 256), BF16),
            VMEM((256, 512), BF16),
            VMEM((2048, 512), BF16),
            pltpu.SemaphoreType.DMA((17,)),
        ],
        compiler_params=params(PROJECT_GRANT),
        cost_estimate=pl.CostEstimate(
            flops=2 * rows * 2048 * 1024, bytes_accessed=8 << 20, transcendentals=0
        ),
        name="project",
    )(place, *small, *pieces, *weights)


def attend_kernel(first, last, tiles, kv_count, place, *refs):
    q_refs, refs = refs[:tiles], refs[tiles:]
    kv_refs, refs = refs[:kv_count], refs[kv_count:]
    before, refs = (None, refs) if first else (refs[:3], refs[3:])
    if last:
        out_ref, refs = refs[0], refs[1:]
    total, sums, shift, buf, held, queries = refs

    def begin():
        if first:
            total[...] = jnp.zeros_like(total)
            sums[...] = jnp.zeros_like(sums)
            shift[...] = jnp.zeros_like(shift)
        else:
            total[...] = before[0][...]
            sums[...] = before[1][...]
            shift[...] = before[2][...]

    begin()
    inner, _, keys = kv_refs[0].shape
    count = kv_count * inner

    def add(t, p, v):
        sums[t] += p.reshape(keys // 8, 8, TILE).sum(axis=0)
        total[t] += dot(v, p.astype(BF16))

    for now in range(count + 1):
        if now < count:
            k = kv_refs[now // inner][now % inner, 0:96, :].T
        for t in range(tiles):
            if now < count:
                buf[now % 2, t] = dot(k, q_refs[t][0:96])
            if now:
                v = kv_refs[(now - 1) // inner][(now - 1) % inner, 96:160, :]
                add(t, jnp.exp2(buf[(now - 1) % 2, t] * LATENT_SCALE - shift[t]), v)

    fits = jnp.max(sums[...]) <= LARGEST
    if first:
        fits = fits & (jnp.min(jnp.sum(sums[...], axis=1)) >= SMALLEST)

    @pl.when(jnp.logical_not(fits))
    def _():
        begin()
        for t in range(tiles):
            queries[t] = q_refs[t][0:96]
        for n, ref in enumerate(kv_refs):
            held[n * inner : (n + 1) * inner] = ref[...]
        if first:
            shift[...] = jnp.full_like(shift, -jnp.inf)

        def again(n, carry):
            t, b = n // count, n % count
            s = dot(held[b, 0:96, :].T, queries[t]) * LATENT_SCALE
            old = shift[t]
            new = jnp.maximum(old, jnp.max(s, axis=0, keepdims=True))
            shrink = jnp.exp2(old - new)
            sums[t] *= shrink
            total[t] *= shrink
            shift[t] = new
            add(t, jnp.exp2(s - new), held[b, 96:160, :])
            return carry

        lax.fori_loop(0, tiles * count, again, 0)

    if last:
        for t in range(tiles):
            line = (place[3] - t + 4) % 4
            out_ref[line] = (total[t] / jnp.sum(sums[t], axis=0, keepdims=True)).astype(BF16)


def attend(place, chunks, kvs, state=None, last=False):
    tiles = len(chunks)
    first = state is None
    inner, depth, keys = kvs[0].shape
    holds = [(tiles, HEAD, TILE), (tiles, 8, TILE), (tiles, 1, TILE)]
    spare = [
        VMEM((2, tiles, keys, TILE), F32),
        VMEM((len(kvs) * inner, depth, keys), BF16),
        VMEM((tiles, NOPE + ROPE, TILE), BF16),
    ]
    if last:
        out_shape = [jax.ShapeDtypeStruct((tiles, HEAD, TILE), BF16)]
        spare = [VMEM(s, F32) for s in holds] + spare
    else:
        out_shape = [jax.ShapeDtypeStruct(s, F32) for s in holds]
    args = (*chunks, *kvs) + (() if first else tuple(state))
    work = tiles * TILE * len(kvs) * inner * keys
    return pl.pallas_call(
        functools.partial(attend_kernel, first, last, tiles, len(kvs)),
        out_shape=out_shape,
        in_specs=[SMEM] + vmem(len(args)),
        out_specs=vmem(len(out_shape)),
        scratch_shapes=spare,
        compiler_params=params(),
        cost_estimate=pl.CostEstimate(
            flops=2 * work * 320, bytes_accessed=3 << 20, transcendentals=work
        ),
        name="attend_last" if last else "attend",
    )(place, *args)


def window_kernel(span_ref, q_ref, kv_ref, left_ref, right_ref, sink_ref, out_ref, ext):
    rows = kv_ref.shape[1]
    ext[:, 0:WINDOW] = left_ref[...]
    ext[:, WINDOW : WINDOW + rows] = kv_ref[...]
    ext[:, WINDOW + rows :] = right_ref[...]
    first_span, last_span = span_ref[0] == 0, span_ref[0] == span_ref[1] - 1
    wide = 3 * WINDOW
    key = lax.broadcasted_iota(jnp.int32, (wide, 2 * WINDOW), 0)
    lane = lax.broadcasted_iota(jnp.int32, (wide, 2 * WINDOW), 1)
    offset = key - jnp.where(lane >= WINDOW, lane - WINDOW, lane)
    near = (offset >= 0) & (offset <= 2 * WINDOW)
    side = lax.broadcasted_iota(jnp.int32, (1, 2 * WINDOW), 1)
    sink = jnp.where(side < WINDOW, sink_ref[0], sink_ref[1]) * LOG2E
    blocks = rows // WINDOW
    for n in range(blocks):
        k = ext[0:64, n * WINDOW : n * WINDOW + wide].T
        v = ext[64:128, n * WINDOW : n * WINDOW + wide]
        allowed = near
        if n == 0:
            allowed = allowed & ((key >= WINDOW) | jnp.logical_not(first_span))
        if n == blocks - 1:
            allowed = allowed & ((key < 2 * WINDOW) | jnp.logical_not(last_span))
        s = jnp.where(allowed, dot(k, q_ref[n]) * WINDOW_SCALE, -jnp.inf)
        top = jnp.maximum(jnp.max(s, axis=0, keepdims=True), sink)
        p = jnp.exp2(s - top)
        denom = jnp.sum(p, axis=0, keepdims=True) + jnp.exp2(sink - top)
        o = (dot(v, p.astype(BF16)) / denom).astype(BF16)
        out_ref[0:64, n * WINDOW : (n + 1) * WINDOW] = o[:, 0:WINDOW]
        out_ref[64:128, n * WINDOW : (n + 1) * WINDOW] = o[:, WINDOW:]


def windowed(span, q, kv, left, right, sink):
    smem = pl.BlockSpec(memory_space=pltpu.SMEM)
    vmem = pl.BlockSpec(memory_space=VMEM)
    rows = kv.shape[1]
    return pl.pallas_call(
        window_kernel,
        out_shape=jax.ShapeDtypeStruct((128, rows), BF16),
        in_specs=[smem, vmem, vmem, vmem, vmem, smem],
        out_specs=vmem,
        scratch_shapes=[VMEM((128, rows + 2 * WINDOW), BF16)],
        cost_estimate=pl.CostEstimate(
            flops=rows * 2 * 384 * 256, bytes_accessed=1 << 20, transcendentals=rows * 768
        ),
        compiler_params=params(),
        name="windowed",
    )(span, q, kv, left, right, sink)


def merge_kernel(place, keep_ref, got_ref, win_ref, wl_ref, ww_ref, *refs):
    own_refs, sib_refs, (mixed, lhs) = refs[:4], refs[4:8], refs[8:]
    chip, core = place[0], place[2]
    for ref, half in ((keep_ref, core), (got_ref, 1 - core)):
        at = pl.ds(pl.multiple_of(half * TILE, TILE), TILE)
        mixed[0:HEAD, at] = ref[0]
        mixed[HEAD : 2 * HEAD, at] = ref[1]
    lhs[:, 0:128] = mixed[...].T
    lhs[:, 128:256] = win_ref[...].T
    rows = lhs[...]
    width = own_refs[0].shape[1]
    for outs, side in ((sib_refs, 1 - core), (own_refs, core)):
        for k in (2, 1, 3, 0):
            start = (2 * ((chip + k) % 4) + side) * width
            at = pl.ds(pl.multiple_of(start, width), width)
            both = jnp.concatenate([wl_ref[:, at], ww_ref[:, at]], axis=0)
            outs[k][...] = dot(rows, both).astype(BF16)


def merge(place, keep, got, win, out_latent, out_window):
    rows = win.shape[1]
    return pl.pallas_call(
        merge_kernel,
        out_shape=[jax.ShapeDtypeStruct((rows, 256), BF16)] * 8,
        in_specs=[SMEM] + vmem(5),
        out_specs=vmem(8),
        scratch_shapes=[VMEM((128, rows), BF16), VMEM((rows, 256), BF16)],
        compiler_params=params(),
        cost_estimate=pl.CostEstimate(
            flops=2 * rows * 256 * 2048, bytes_accessed=4 << 20, transcendentals=0
        ),
        name="merge",
    )(place, keep, got, win, out_latent, out_window)


SWAP = [(0, 1), (1, 0)]


def shifted(value, axis, by):
    count = lax.axis_size(axis)
    return lax.ppermute(value, axis, [(i, (i + by) % count) for i in range(count)])


def other_core(value):
    return lax.ppermute(value, "c", SWAP)


def ring_step(value):
    count = lax.axis_size("z")
    up = [(2 * i, 2 * ((i + 1) % count)) for i in range(count)]
    down = [(2 * i + 1, 2 * ((i - 1) % count) + 1) for i in range(count)]
    return lax.ppermute(value, ("z", "c"), up + down)


def head_routes(turn):
    routes = []
    for y in range(4):
        d = (y + turn) % 4
        for c in range(2):
            routes.append((2 * y + c, 2 * (2 * c + d // 2) + d % 2))
    return routes


def shards(
    inputs,
    norm_gain,
    latent_query,
    latent_down,
    rope_down,
    latent_gain,
    latent_up,
    window_query,
    window_key,
    window_value,
    sink_logit,
    out_latent,
    out_window,
):
    rows = inputs.shape[0]
    core = lax.axis_index("c")
    line = lax.axis_index("y")
    span = lax.axis_index(("z", "y"))
    spans = lax.axis_size(("z", "y"))
    slot = 2 * (line % 2) + core
    place = jnp.stack([lax.axis_index("x"), line, core, slot]).astype(jnp.int32)

    before = shifted(inputs, "x", 1)
    after = shifted(inputs, "x", -1)
    far_low = shifted(before[:TILE], "x", 1)
    far_high = shifted(after[TILE:], "x", -1)
    pieces = []
    for array in (inputs, before, after, far_low, far_high):
        pieces += [array, other_core(array)]
    powers = np.arange(0, HEAD, 2).astype(np.float64) / HEAD
    inverse = 1.0 / 10000.0**powers
    inverse = jnp.asarray(np.concatenate([inverse, inverse[::2]]), F32)
    positions = (span * rows + jnp.arange(rows)).astype(F32)
    angles = inverse[:, None] * positions[None, :]
    tables = jnp.cos(angles), jnp.sin(angles)
    *chunks, wq, wkv = project(
        place,
        (norm_gain.reshape(8, 1, 256), latent_gain[None], *tables),
        pieces,
        (
            latent_query.T,
            rope_down.T,
            window_key.T,
            window_value.T,
            window_query,
            latent_up,
            latent_down,
        ),
        rows,
    )
    mine = []
    for r, chunk in enumerate(chunks):
        mine.append(lax.ppermute(chunk, ("y", "c"), head_routes(r)))
    left = lax.ppermute(
        wkv[:, rows - WINDOW :], ("z", "y"), [(i, i + 1) for i in range(spans - 1)]
    )
    right = lax.ppermute(
        wkv[:, :WINDOW], ("z", "y"), [(i + 1, i) for i in range(spans - 1)]
    )
    where = jnp.stack([span, spans]).astype(jnp.int32)
    win = windowed(where, wq, wkv, left, right, sink_logit)

    low = jnp.stack([c[96:256] for c in mine])
    high = other_core(low)
    state = None
    waiting = None
    for n in range(4):
        arriving = ring_step(low)
        blocks = [low]
        if n:
            blocks.append(other_core(low))
            if n > 1:
                state = attend(place, mine, waiting, state)
        state_low = functools.partial(attend, place, mine, blocks)
        waiting = [high]
        if n:
            waiting.append(other_core(high))
        if n < 3:
            high = ring_step(high)
        state = state_low(state)
        if n == 0:
            state = attend(place, mine, waiting, state)
        low = arriving
    blocks = [low, other_core(low)]
    state = attend(place, mine, waiting, state)
    (mixed,) = attend(place, mine, blocks, state, last=True)

    back = lax.all_to_all(mixed, "y", 0, 0, tiled=True)
    pairs = back.reshape(2, 2, HEAD, TILE)
    keep = lax.dynamic_index_in_dim(pairs, core, 0, keepdims=False)
    give = lax.dynamic_index_in_dim(pairs, 1 - core, 0, keepdims=False)
    sums = merge(place, keep, other_core(give), win, out_latent, out_window)
    total = 0
    for k in (2, 1, 3, 0):
        own, sibling = sums[k], other_core(sums[4 + k])
        both = own.astype(F32) + sibling.astype(F32)
        if k:
            both = shifted(both.astype(BF16), "x", k).astype(F32)
        total = total + both
    return total.astype(BF16)


def solution(mesh):
    shape = (8, 4, 4, 2)
    torus = Mesh(mesh.devices.reshape(shape), ("z", "y", "x", "c"))
    sp, tp = ("z", "y"), ("x", "c")
    in_specs = (
        P(sp, tp),
        P(),
        P(None, tp),
        P(),
        P(),
        P(),
        P(None, tp),
        P(None, tp),
        P(None, tp),
        P(None, tp),
        P(tp),
        P(tp, None),
        P(tp, None),
    )
    return jax.shard_map(
        shards, mesh=torus, in_specs=in_specs, out_specs=P(sp, tp), check_vma=False
    )
```

```python
import functools
import math

import jax
import jax.numpy as jnp
import numpy as np
from jax import lax
from jax.experimental import pallas as pl
from jax.experimental.pallas import tpu as pltpu
from jax.sharding import Mesh
from jax.sharding import PartitionSpec as P


NOPE = 64
ROPE = 32
HEAD = 64
WINDOW = 128
TILE = 256
epsilon = 1e-06
LOG2E = math.log2(math.e)
LATENT_SCALE = LOG2E * (NOPE + ROPE) ** (-0.5)
WINDOW_SCALE = LOG2E * HEAD ** (-0.5)
GRANT = 12 << 20
PROJECT_GRANT = 60 << 20
UNROLL = 4
SMALLEST = 2.0**-60
LARGEST = 2.0**100
F32 = jnp.float32
BF16 = jnp.bfloat16
VMEM = pltpu.VMEM


NT = (((1,), (1,)), ((), ()))


def dot(a, b):
    return jnp.dot(a, b, preferred_element_type=F32)


def dot_nt(a, b):
    return lax.dot_general(a, b, NT, preferred_element_type=F32)


def rotate(v, cos, sin):
    half = v.shape[0] // 2
    a, b = v[:half], v[half:]
    return jnp.concatenate([a * cos - b * sin, b * cos + a * sin], axis=0)


def params(grant=GRANT):
    return pltpu.CompilerParams(vmem_limit_bytes=grant)


def vmem(count):
    return [pl.BlockSpec(memory_space=VMEM)] * count


SMEM = pl.BlockSpec(memory_space=pltpu.SMEM)
HBM = pl.BlockSpec(memory_space=pltpu.HBM)
ANY = pl.BlockSpec(memory_space=pl.ANY)


def project_kernel(place, gain_ref, lgain_ref, cos_ref, sin_ref, *refs):
    x_hbm, (lq_hbm, rope_hbm, wk_hbm, wv_hbm, wq_hbm, up_hbm, down_hbm), refs = (
        refs[:10],
        refs[10:17],
        refs[17:],
    )
    chunk_refs, (wq_out, wkv_out), refs = refs[:4], refs[4:6], refs[6:]
    xs, hid, rows_ref, wq_ref, up_ref, up_rows, down_ref, sems = refs
    chip, line, core = place[0], place[1], place[2]
    blocks, _, width = xs.shape
    targets = [xs.at[n] for n in range(6)]
    for n in (6, 7):
        targets.insert(len(targets), xs.at[n, 0:TILE])
    for n in (6, 7):
        targets.insert(len(targets), xs.at[n, TILE : 2 * TILE])
    targets += [
        rows_ref.at[0:192],
        rows_ref.at[192:224],
        rows_ref.at[224:288],
        rows_ref.at[288:352],
        wq_ref,
        up_ref,
        down_ref,
    ]
    sources = [*x_hbm, lq_hbm, rope_hbm, wk_hbm, wv_hbm, wq_hbm, up_hbm, down_hbm]
    copies = [
        pltpu.make_async_copy(a, b, sems.at[n]) for n, (a, b) in enumerate(zip(sources, targets))
    ]
    for copy in copies:
        copy.start()
    for copy in copies[:10]:
        copy.wait()

    def normalize(part, carry):
        at = pl.ds(pl.multiple_of(part * TILE, TILE), TILE)
        total = jnp.zeros((TILE, 1), F32)
        for n in range(blocks):
            x = xs[n, at].astype(F32)
            total += jnp.sum(x * x, axis=1, keepdims=True)
        scale = lax.rsqrt(total / (blocks * width) + epsilon)
        for n in range(blocks):
            block = 2 * ((chip + (0, 3, 1, 2)[n // 2]) % 4) + (core + n) % 2
            x = xs[n, at].astype(F32)
            hid[part, :, pl.ds(pl.multiple_of(block * width, width), width)] = (
                x * scale * gain_ref[block]
            ).astype(BF16)
        return carry

    lax.fori_loop(0, 2, normalize, 0)
    for copy in copies[10:]:
        copy.wait()
    rows_ref[352:480] = wq_ref[...].T
    up_rows[...] = up_ref[...].T

    def heads(part, carry):
        at = pl.ds(pl.multiple_of(part * TILE, TILE), TILE)
        hidden = hid[part]
        cos64, sin64 = cos_ref[0:32, at], sin_ref[0:32, at]
        cos32, sin32 = cos_ref[32:48, at], sin_ref[32:48, at]
        raw = dot(hidden, down_ref[...])
        mean = jnp.mean(raw * raw, axis=1, keepdims=True)
        latent = (raw * lax.rsqrt(mean + epsilon) * lgain_ref[...]).astype(BF16)
        together = dot_nt(rows_ref[...], hidden)
        expanded = dot_nt(up_rows[...], latent).astype(BF16)
        queries = together[0:192]
        shared = rotate(together[192:224], cos32, sin32).astype(BF16)
        for h in range(2):
            base = h * (NOPE + ROPE)
            own = h * (NOPE + HEAD)
            plain = queries[base : base + NOPE].astype(BF16)
            turned = rotate(queries[base + NOPE : base + NOPE + ROPE], cos32, sin32).astype(BF16)
            turn = (2 * h + part - line + 4) % 4
            for r, out in enumerate(chunk_refs):

                @pl.when(turn == r)
                def _():
                    out[0:64] = plain
                    out[64:96] = turned
                    out[96:160] = expanded[own : own + NOPE]
                    out[160:192] = shared
                    out[192:256] = expanded[own + NOPE : own + NOPE + HEAD]

        window_q = together[352:480]
        first = rotate(window_q[0:64], cos64, sin64).astype(BF16)
        second = rotate(window_q[64:128], cos64, sin64).astype(BF16)
        for n in range(2):
            cut = slice(n * WINDOW, (n + 1) * WINDOW)
            wq_out[2 * part + n, :, 0:WINDOW] = first[:, cut]
            wq_out[2 * part + n, :, WINDOW : 2 * WINDOW] = second[:, cut]
        wkv_out[0:64, at] = rotate(together[224:288], cos64, sin64).astype(BF16)
        wkv_out[64:128, at] = together[288:352].astype(BF16)
        return carry

    lax.fori_loop(0, 2, heads, 0)


def project(place, small, pieces, weights, rows):
    return pl.pallas_call(
        project_kernel,
        out_shape=[jax.ShapeDtypeStruct((256, TILE), BF16)] * 4
        + [
            jax.ShapeDtypeStruct((rows // WINDOW, 64, 2 * WINDOW), BF16),
            jax.ShapeDtypeStruct((128, rows), BF16),
        ],
        in_specs=[SMEM] + vmem(len(small)) + [HBM] * (len(pieces) + len(weights)),
        out_specs=vmem(6),
        scratch_shapes=[
            VMEM((8, rows, 256), BF16),
            VMEM((2, TILE, 2048), BF16),
            VMEM((480, 2048), BF16),
            VMEM((2048, 128), BF16),
            VMEM((512, 256), BF16),
            VMEM((256, 512), BF16),
            VMEM((2048, 512), BF16),
            pltpu.SemaphoreType.DMA((17,)),
        ],
        compiler_params=params(PROJECT_GRANT),
        cost_estimate=pl.CostEstimate(
            flops=2 * rows * 2048 * 1024, bytes_accessed=8 << 20, transcendentals=0
        ),
        name="project",
    )(place, *small, *pieces, *weights)


def attend_kernel(first, last, tiles, kv_count, unroll, place, *refs):
    q_refs, refs = refs[:tiles], refs[tiles:]
    kv_refs, refs = refs[:kv_count], refs[kv_count:]
    before, refs = (None, refs) if first else (refs[:3], refs[3:])
    if last:
        out_ref, refs = refs[0], refs[1:]
    total, sums, shift, buf, held, queries = refs

    def begin():
        if first:
            total[...] = jnp.zeros_like(total)
            sums[...] = jnp.zeros_like(sums)
            shift[...] = jnp.zeros_like(shift)
        else:
            total[...] = before[0][...]
            sums[...] = before[1][...]
            shift[...] = before[2][...]

    begin()
    inner, _, keys = kv_refs[0].shape
    count = kv_count * inner

    def add(t, p, v):
        sums[t] += p.reshape(keys // 8, 8, TILE).sum(axis=0)
        total[t] += dot(v, p.astype(BF16))

    for n, ref in enumerate(kv_refs):
        held[n * inner : (n + 1) * inner] = ref[...]
    for t in range(tiles):
        buf[0, t] = dot(held[0, 0:96, :].T, q_refs[t][0:96])

    def step(i, carry):
        for b in range(unroll):
            now = unroll * i + b
            k = held[jnp.minimum(now + 1, count - 1), 0:96, :].T
            v = held[now, 96:160, :]
            for t in range(tiles):
                buf[(b + 1) % 2, t] = dot(k, q_refs[t][0:96])
                add(t, jnp.exp2(buf[b % 2, t] * LATENT_SCALE - shift[t]), v)
        return carry

    lax.fori_loop(0, count // unroll, step, 0)

    fits = jnp.max(sums[...]) <= LARGEST
    if first:
        fits = fits & (jnp.min(jnp.sum(sums[...], axis=1)) >= SMALLEST)

    @pl.when(jnp.logical_not(fits))
    def _():
        begin()
        for t in range(tiles):
            queries[t] = q_refs[t][0:96]
        if first:
            shift[...] = jnp.full_like(shift, -jnp.inf)

        def again(n, carry):
            t, b = n // count, n % count
            s = dot(held[b, 0:96, :].T, queries[t]) * LATENT_SCALE
            old = shift[t]
            new = jnp.maximum(old, jnp.max(s, axis=0, keepdims=True))
            shrink = jnp.exp2(old - new)
            sums[t] *= shrink
            total[t] *= shrink
            shift[t] = new
            add(t, jnp.exp2(s - new), held[b, 96:160, :])
            return carry

        lax.fori_loop(0, tiles * count, again, 0)

    if last:
        for t in range(tiles):
            line = (place[3] - t + 4) % 4
            out_ref[line] = (total[t] / jnp.sum(sums[t], axis=0, keepdims=True)).astype(BF16)


def attend(place, chunks, kvs, state=None, last=False, unroll=UNROLL):
    tiles = len(chunks)
    first = state is None
    inner, depth, keys = kvs[0].shape
    holds = [(tiles, HEAD, TILE), (tiles, 8, TILE), (tiles, 1, TILE)]
    spare = [
        VMEM((2, tiles, keys, TILE), F32),
        VMEM((len(kvs) * inner, depth, keys), BF16),
        VMEM((tiles, NOPE + ROPE, TILE), BF16),
    ]
    if last:
        out_shape = [jax.ShapeDtypeStruct((tiles, HEAD, TILE), BF16)]
        spare = [VMEM(s, F32) for s in holds] + spare
    else:
        out_shape = [jax.ShapeDtypeStruct(s, F32) for s in holds]
    args = (*chunks, *kvs) + (() if first else tuple(state))
    work = tiles * TILE * len(kvs) * inner * keys
    return pl.pallas_call(
        functools.partial(attend_kernel, first, last, tiles, len(kvs), unroll),
        out_shape=out_shape,
        in_specs=[SMEM] + vmem(len(args)),
        out_specs=vmem(len(out_shape)),
        scratch_shapes=spare,
        compiler_params=params(),
        cost_estimate=pl.CostEstimate(
            flops=2 * work * 320, bytes_accessed=3 << 20, transcendentals=work
        ),
        name="attend_last" if last else "attend",
    )(place, *args)


def window_kernel(span_ref, q_ref, kv_ref, left_ref, right_ref, sink_ref, out_ref, ext):
    rows = kv_ref.shape[1]
    ext[:, 0:WINDOW] = left_ref[...]
    ext[:, WINDOW : WINDOW + rows] = kv_ref[...]
    ext[:, WINDOW + rows :] = right_ref[...]
    first_span, last_span = span_ref[0] == 0, span_ref[0] == span_ref[1] - 1
    wide = 3 * WINDOW
    key = lax.broadcasted_iota(jnp.int32, (wide, 2 * WINDOW), 0)
    lane = lax.broadcasted_iota(jnp.int32, (wide, 2 * WINDOW), 1)
    offset = key - jnp.where(lane >= WINDOW, lane - WINDOW, lane)
    near = (offset >= 0) & (offset <= 2 * WINDOW)
    side = lax.broadcasted_iota(jnp.int32, (1, 2 * WINDOW), 1)
    sink = jnp.where(side < WINDOW, sink_ref[0], sink_ref[1]) * LOG2E
    blocks = rows // WINDOW
    for n in range(blocks):
        k = ext[0:64, n * WINDOW : n * WINDOW + wide].T
        v = ext[64:128, n * WINDOW : n * WINDOW + wide]
        allowed = near
        if n == 0:
            allowed = allowed & ((key >= WINDOW) | jnp.logical_not(first_span))
        if n == blocks - 1:
            allowed = allowed & ((key < 2 * WINDOW) | jnp.logical_not(last_span))
        s = jnp.where(allowed, dot(k, q_ref[n]) * WINDOW_SCALE, -jnp.inf)
        top = jnp.maximum(jnp.max(s, axis=0, keepdims=True), sink)
        p = jnp.exp2(s - top)
        denom = jnp.sum(p, axis=0, keepdims=True) + jnp.exp2(sink - top)
        o = (dot(v, p.astype(BF16)) / denom).astype(BF16)
        out_ref[0:64, n * WINDOW : (n + 1) * WINDOW] = o[:, 0:WINDOW]
        out_ref[64:128, n * WINDOW : (n + 1) * WINDOW] = o[:, WINDOW:]


def windowed(span, q, kv, left, right, sink):
    smem = pl.BlockSpec(memory_space=pltpu.SMEM)
    vmem = pl.BlockSpec(memory_space=VMEM)
    rows = kv.shape[1]
    return pl.pallas_call(
        window_kernel,
        out_shape=jax.ShapeDtypeStruct((128, rows), BF16),
        in_specs=[smem, vmem, vmem, vmem, vmem, smem],
        out_specs=vmem,
        scratch_shapes=[VMEM((128, rows + 2 * WINDOW), BF16)],
        cost_estimate=pl.CostEstimate(
            flops=rows * 2 * 384 * 256, bytes_accessed=1 << 20, transcendentals=rows * 768
        ),
        compiler_params=params(),
        name="windowed",
    )(span, q, kv, left, right, sink)


def merge_kernel(place, keep_ref, got_ref, win_ref, wl_ref, ww_ref, *refs):
    own_refs, sib_ref, (mixed, lhs) = refs[:4], refs[4], refs[5:]
    sib_refs = [sib_ref.at[k] for k in range(4)]
    chip, core = place[0], place[2]
    for ref, half in ((keep_ref, core), (got_ref, 1 - core)):
        at = pl.ds(pl.multiple_of(half * TILE, TILE), TILE)
        mixed[0:HEAD, at] = ref[0]
        mixed[HEAD : 2 * HEAD, at] = ref[1]
    lhs[:, 0:128] = mixed[...].T
    lhs[:, 128:256] = win_ref[...].T
    rows = lhs[...]
    width = own_refs[0].shape[1]
    for outs, side in ((sib_refs, 1 - core), (own_refs, core)):
        for k in (2, 1, 3, 0):
            start = (2 * ((chip + k) % 4) + side) * width
            at = pl.ds(pl.multiple_of(start, width), width)
            both = jnp.concatenate([wl_ref[:, at], ww_ref[:, at]], axis=0)
            outs[k][...] = dot(rows, both).astype(BF16)


def merge(place, keep, got, win, out_latent, out_window):
    rows = win.shape[1]
    return pl.pallas_call(
        merge_kernel,
        out_shape=[jax.ShapeDtypeStruct((rows, 256), BF16)] * 4
        + [jax.ShapeDtypeStruct((4, rows, 256), BF16)],
        in_specs=[SMEM] + vmem(5),
        out_specs=vmem(5),
        scratch_shapes=[VMEM((128, rows), BF16), VMEM((rows, 256), BF16)],
        compiler_params=params(),
        cost_estimate=pl.CostEstimate(
            flops=2 * rows * 256 * 2048, bytes_accessed=4 << 20, transcendentals=0
        ),
        name="merge",
    )(place, keep, got, win, out_latent, out_window)


SWAP = [(0, 1), (1, 0)]


def shifted(value, axis, by):
    count = lax.axis_size(axis)
    return lax.ppermute(value, axis, [(i, (i + by) % count) for i in range(count)])


def other_core(value):
    return lax.ppermute(value, "c", SWAP)


def ring_step(value):
    count = lax.axis_size("z")
    up = [(2 * i, 2 * ((i + 1) % count)) for i in range(count)]
    down = [(2 * i + 1, 2 * ((i - 1) % count) + 1) for i in range(count)]
    return lax.ppermute(value, ("z", "c"), up + down)


def head_routes(turn):
    routes = []
    for y in range(4):
        d = (y + turn) % 4
        for c in range(2):
            routes.append((2 * y + c, 2 * (2 * c + d // 2) + d % 2))
    return routes


def shards(
    inputs,
    norm_gain,
    latent_query,
    latent_down,
    rope_down,
    latent_gain,
    latent_up,
    window_query,
    window_key,
    window_value,
    sink_logit,
    out_latent,
    out_window,
):
    rows = inputs.shape[0]
    core = lax.axis_index("c")
    line = lax.axis_index("y")
    span = lax.axis_index(("z", "y"))
    spans = lax.axis_size(("z", "y"))
    slot = 2 * (line % 2) + core
    place = jnp.stack([lax.axis_index("x"), line, core, slot]).astype(jnp.int32)

    before = shifted(inputs, "x", 1)
    after = shifted(inputs, "x", -1)
    far_low = shifted(before[:TILE], "x", 1)
    far_high = shifted(after[TILE:], "x", -1)
    pieces = []
    for array in (inputs, before, after, far_low, far_high):
        pieces += [array, other_core(array)]
    powers = np.arange(0, HEAD, 2).astype(np.float64) / HEAD
    inverse = 1.0 / 10000.0**powers
    inverse = jnp.asarray(np.concatenate([inverse, inverse[::2]]), F32)
    positions = (span * rows + jnp.arange(rows)).astype(F32)
    angles = inverse[:, None] * positions[None, :]
    tables = jnp.cos(angles), jnp.sin(angles)
    *chunks, wq, wkv = project(
        place,
        (norm_gain.reshape(8, 1, 256), latent_gain[None], *tables),
        pieces,
        (
            latent_query.T,
            rope_down.T,
            window_key.T,
            window_value.T,
            window_query,
            latent_up,
            latent_down,
        ),
        rows,
    )
    mine = []
    for r, chunk in enumerate(chunks):
        mine.append(lax.ppermute(chunk, ("y", "c"), head_routes(r)))
    left = lax.ppermute(
        wkv[:, rows - WINDOW :], ("z", "y"), [(i, i + 1) for i in range(spans - 1)]
    )
    right = lax.ppermute(
        wkv[:, :WINDOW], ("z", "y"), [(i + 1, i) for i in range(spans - 1)]
    )
    where = jnp.stack([span, spans]).astype(jnp.int32)
    win = windowed(where, wq, wkv, left, right, sink_logit)

    low = jnp.stack([c[96:256] for c in mine])
    high = other_core(low)
    arriving = ring_step(low)
    state = attend(place, mine, [low, high], unroll=2)
    high = ring_step(high)
    low = arriving
    waiting = None
    for n in (1, 2, 3):
        arriving = ring_step(low)
        blocks = [low, other_core(low)]
        if waiting:
            state = attend(place, mine, waiting, state, unroll=2 if n == 2 else UNROLL)
        waiting = [high, other_core(high)]
        if n < 3:
            high = ring_step(high)
        state = attend(place, mine, blocks, state, unroll=2 if n == 1 else UNROLL)
        low = arriving
    blocks = [low, other_core(low)]
    state = attend(place, mine, waiting, state)
    (mixed,) = attend(place, mine, blocks, state, last=True)

    back = lax.all_to_all(mixed, "y", 0, 0, tiled=True)
    pairs = back.reshape(2, 2, HEAD, TILE)
    keep = lax.dynamic_index_in_dim(pairs, core, 0, keepdims=False)
    give = lax.dynamic_index_in_dim(pairs, 1 - core, 0, keepdims=False)
    sums = merge(place, keep, other_core(give), win, out_latent, out_window)
    siblings = other_core(sums[4])
    total = 0
    for k in (2, 1, 3, 0):
        both = sums[k].astype(F32) + siblings[k].astype(F32)
        if k:
            both = shifted(both.astype(BF16), "x", k).astype(F32)
        total = total + both
    return total.astype(BF16)


def solution(mesh):
    shape = (8, 4, 4, 2)
    torus = Mesh(mesh.devices.reshape(shape), ("z", "y", "x", "c"))
    sp, tp = ("z", "y"), ("x", "c")
    in_specs = (
        P(sp, tp),
        P(),
        P(None, tp),
        P(),
        P(),
        P(),
        P(None, tp),
        P(None, tp),
        P(None, tp),
        P(None, tp),
        P(tp),
        P(tp, None),
        P(tp, None),
    )
    return jax.shard_map(
        shards, mesh=torus, in_specs=in_specs, out_specs=P(sp, tp), check_vma=False
    )
```

```python
import functools
import math

import jax
import jax.numpy as jnp
import numpy as np
from jax import lax
from jax.experimental import pallas as pl
from jax.experimental.pallas import tpu as pltpu
from jax.sharding import Mesh
from jax.sharding import PartitionSpec as P


NOPE = 64
ROPE = 32
HEAD = 64
WINDOW = 128
TILE = 256
epsilon = 1e-06
LOG2E = math.log2(math.e)
LATENT_SCALE = LOG2E * (NOPE + ROPE) ** (-0.5)
WINDOW_SCALE = LOG2E * HEAD ** (-0.5)
GRANT = 12 << 20
PROJECT_GRANT = 60 << 20
UNROLL = 4
SMALLEST = 2.0**-60
LARGEST = 2.0**100
F32 = jnp.float32
BF16 = jnp.bfloat16
VMEM = pltpu.VMEM


NT = (((1,), (1,)), ((), ()))


def dot(a, b):
    return jnp.dot(a, b, preferred_element_type=F32)


def dot_nt(a, b):
    return lax.dot_general(a, b, NT, preferred_element_type=F32)


def rotate(v, cos, sin):
    half = v.shape[0] // 2
    a, b = v[:half], v[half:]
    return jnp.concatenate([a * cos - b * sin, b * cos + a * sin], axis=0)


def params(grant=GRANT):
    return pltpu.CompilerParams(vmem_limit_bytes=grant)


def vmem(count):
    return [pl.BlockSpec(memory_space=VMEM)] * count


SMEM = pl.BlockSpec(memory_space=pltpu.SMEM)
HBM = pl.BlockSpec(memory_space=pltpu.HBM)
ANY = pl.BlockSpec(memory_space=pl.ANY)


def project_kernel(place, gain_ref, lgain_ref, cos_ref, sin_ref, *refs):
    x_hbm, (lq_hbm, rope_hbm, wk_hbm, wv_hbm, wq_hbm, up_hbm, down_hbm), refs = (
        refs[:10],
        refs[10:17],
        refs[17:],
    )
    chunk_refs, (wq_out, wkv_out), refs = refs[:2], refs[2:4], refs[4:]
    xs, hid, rows_ref, wq_ref, up_ref, up_rows, down_ref, sems = refs
    chip, line, core = place[0], place[1], place[2]
    blocks, _, width = xs.shape
    targets = [xs.at[n] for n in range(6)]
    for n in (6, 7):
        targets.insert(len(targets), xs.at[n, 0:TILE])
    for n in (6, 7):
        targets.insert(len(targets), xs.at[n, TILE : 2 * TILE])
    targets += [
        rows_ref.at[0:192],
        rows_ref.at[192:224],
        rows_ref.at[224:288],
        rows_ref.at[288:352],
        wq_ref,
        up_ref,
        down_ref,
    ]
    sources = [*x_hbm, lq_hbm, rope_hbm, wk_hbm, wv_hbm, wq_hbm, up_hbm, down_hbm]
    copies = [
        pltpu.make_async_copy(a, b, sems.at[n]) for n, (a, b) in enumerate(zip(sources, targets))
    ]
    for copy in copies:
        copy.start()
    for copy in copies[:10]:
        copy.wait()

    def normalize(part, carry):
        at = pl.ds(pl.multiple_of(part * TILE, TILE), TILE)
        total = jnp.zeros((TILE, 1), F32)
        for n in range(blocks):
            x = xs[n, at].astype(F32)
            total += jnp.sum(x * x, axis=1, keepdims=True)
        scale = lax.rsqrt(total / (blocks * width) + epsilon)
        for n in range(blocks):
            block = 2 * ((chip + (0, 3, 1, 2)[n // 2]) % 4) + (core + n) % 2
            x = xs[n, at].astype(F32)
            hid[part, :, pl.ds(pl.multiple_of(block * width, width), width)] = (
                x * scale * gain_ref[block]
            ).astype(BF16)
        return carry

    lax.fori_loop(0, 2, normalize, 0)
    for copy in copies[10:]:
        copy.wait()
    rows_ref[352:480] = wq_ref[...].T
    up_rows[...] = up_ref[...].T

    def heads(part, carry):
        at = pl.ds(pl.multiple_of(part * TILE, TILE), TILE)
        hidden = hid[part]
        cos64, sin64 = cos_ref[0:32, at], sin_ref[0:32, at]
        cos32, sin32 = cos_ref[32:48, at], sin_ref[32:48, at]
        raw = dot(hidden, down_ref[...])
        mean = jnp.mean(raw * raw, axis=1, keepdims=True)
        latent = (raw * lax.rsqrt(mean + epsilon) * lgain_ref[...]).astype(BF16)
        together = dot_nt(rows_ref[...], hidden)
        expanded = dot_nt(up_rows[...], latent).astype(BF16)
        queries = together[0:192]
        shared = rotate(together[192:224], cos32, sin32).astype(BF16)
        for h in range(2):
            base = h * (NOPE + ROPE)
            own = h * (NOPE + HEAD)
            plain = queries[base : base + NOPE].astype(BF16)
            turned = rotate(queries[base + NOPE : base + NOPE + ROPE], cos32, sin32).astype(BF16)
            turn = (h + line) % 2
            for r, out in enumerate(chunk_refs):

                @pl.when(turn == r)
                def _():
                    out[part, 0:64] = plain
                    out[part, 64:96] = turned
                    out[part, 96:160] = expanded[own : own + NOPE]
                    out[part, 160:192] = shared
                    out[part, 192:256] = expanded[own + NOPE : own + NOPE + HEAD]

        window_q = together[352:480]
        first = rotate(window_q[0:64], cos64, sin64).astype(BF16)
        second = rotate(window_q[64:128], cos64, sin64).astype(BF16)
        for n in range(2):
            cut = slice(n * WINDOW, (n + 1) * WINDOW)
            wq_out[2 * part + n, :, 0:WINDOW] = first[:, cut]
            wq_out[2 * part + n, :, WINDOW : 2 * WINDOW] = second[:, cut]
        wkv_out[0:64, at] = rotate(together[224:288], cos64, sin64).astype(BF16)
        wkv_out[64:128, at] = together[288:352].astype(BF16)
        return carry

    lax.fori_loop(0, 2, heads, 0)


def project(place, small, pieces, weights, rows):
    return pl.pallas_call(
        project_kernel,
        out_shape=[jax.ShapeDtypeStruct((2, 256, TILE), BF16)] * 2
        + [
            jax.ShapeDtypeStruct((rows // WINDOW, 64, 2 * WINDOW), BF16),
            jax.ShapeDtypeStruct((128, rows), BF16),
        ],
        in_specs=[SMEM] + vmem(len(small)) + [HBM] * (len(pieces) + len(weights)),
        out_specs=vmem(4),
        scratch_shapes=[
            VMEM((8, rows, 256), BF16),
            VMEM((2, TILE, 2048), BF16),
            VMEM((480, 2048), BF16),
            VMEM((2048, 128), BF16),
            VMEM((512, 256), BF16),
            VMEM((256, 512), BF16),
            VMEM((2048, 512), BF16),
            pltpu.SemaphoreType.DMA((17,)),
        ],
        compiler_params=params(PROJECT_GRANT),
        cost_estimate=pl.CostEstimate(
            flops=2 * rows * 2048 * 1024, bytes_accessed=8 << 20, transcendentals=0
        ),
        name="project",
    )(place, *small, *pieces, *weights)


def attend_kernel(first, last, tiles, kv_count, unroll, place, *refs):
    q_refs, refs = [refs[t // 2].at[t % 2] for t in range(tiles)], refs[tiles // 2 :]
    kv_refs, refs = refs[:kv_count], refs[kv_count:]
    before, refs = (None, refs) if first else (refs[:3], refs[3:])
    if last:
        out_ref, refs = refs[0], refs[1:]
    total, sums, shift, buf, held, queries = refs

    def begin():
        if first:
            total[...] = jnp.zeros_like(total)
            sums[...] = jnp.zeros_like(sums)
            shift[...] = jnp.zeros_like(shift)
        else:
            total[...] = before[0][...]
            sums[...] = before[1][...]
            shift[...] = before[2][...]

    begin()
    inner, _, keys = kv_refs[0].shape
    count = kv_count * inner

    def add(t, p, v):
        sums[t] += p.reshape(keys // 8, 8, TILE).sum(axis=0)
        total[t] += dot(v, p.astype(BF16))

    for n, ref in enumerate(kv_refs):
        held[n * inner : (n + 1) * inner] = ref[...]
    for t in range(tiles):
        buf[0, t] = dot(held[0, 0:96, :].T, q_refs[t][0:96])

    def step(i, carry):
        for b in range(unroll):
            now = unroll * i + b
            k = held[jnp.minimum(now + 1, count - 1), 0:96, :].T
            v = held[now, 96:160, :]
            for t in range(tiles):
                buf[(b + 1) % 2, t] = dot(k, q_refs[t][0:96])
                add(t, jnp.exp2(buf[b % 2, t] * LATENT_SCALE - shift[t]), v)
        return carry

    lax.fori_loop(0, count // unroll, step, 0)

    fits = jnp.max(sums[...]) <= LARGEST
    if first:
        fits = fits & (jnp.min(jnp.sum(sums[...], axis=1)) >= SMALLEST)

    @pl.when(jnp.logical_not(fits))
    def _():
        begin()
        for t in range(tiles):
            queries[t] = q_refs[t][0:96]
        if first:
            shift[...] = jnp.full_like(shift, -jnp.inf)

        def again(n, carry):
            t, b = n // count, n % count
            s = dot(held[b, 0:96, :].T, queries[t]) * LATENT_SCALE
            old = shift[t]
            new = jnp.maximum(old, jnp.max(s, axis=0, keepdims=True))
            shrink = jnp.exp2(old - new)
            sums[t] *= shrink
            total[t] *= shrink
            shift[t] = new
            add(t, jnp.exp2(s - new), held[b, 96:160, :])
            return carry

        lax.fori_loop(0, tiles * count, again, 0)

    if last:
        for t in range(tiles):
            line = 2 * ((place[2] + t // 2) % 2) + (place[1] + t) % 2
            out_ref[line] = (total[t] / jnp.sum(sums[t], axis=0, keepdims=True)).astype(BF16)


def attend(place, chunks, kvs, state=None, last=False, unroll=UNROLL):
    tiles = 2 * len(chunks)
    first = state is None
    inner, depth, keys = kvs[0].shape
    holds = [(tiles, HEAD, TILE), (tiles, 8, TILE), (tiles, 1, TILE)]
    spare = [
        VMEM((2, tiles, keys, TILE), F32),
        VMEM((len(kvs) * inner, depth, keys), BF16),
        VMEM((tiles, NOPE + ROPE, TILE), BF16),
    ]
    if last:
        out_shape = [jax.ShapeDtypeStruct((tiles, HEAD, TILE), BF16)]
        spare = [VMEM(s, F32) for s in holds] + spare
    else:
        out_shape = [jax.ShapeDtypeStruct(s, F32) for s in holds]
    args = (*chunks, *kvs) + (() if first else tuple(state))
    work = tiles * TILE * len(kvs) * inner * keys
    return pl.pallas_call(
        functools.partial(attend_kernel, first, last, tiles, len(kvs), unroll),
        out_shape=out_shape,
        in_specs=[SMEM] + vmem(len(args)),
        out_specs=vmem(len(out_shape)),
        scratch_shapes=spare,
        compiler_params=params(),
        cost_estimate=pl.CostEstimate(
            flops=2 * work * 320, bytes_accessed=3 << 20, transcendentals=work
        ),
        name="attend_last" if last else "attend",
    )(place, *args)


def window_kernel(span_ref, q_ref, kv_ref, left_ref, right_ref, sink_ref, out_ref, ext):
    rows = kv_ref.shape[1]
    ext[:, 0:WINDOW] = left_ref[...]
    ext[:, WINDOW : WINDOW + rows] = kv_ref[...]
    ext[:, WINDOW + rows :] = right_ref[...]
    first_span, last_span = span_ref[0] == 0, span_ref[0] == span_ref[1] - 1
    wide = 3 * WINDOW
    key = lax.broadcasted_iota(jnp.int32, (wide, 2 * WINDOW), 0)
    lane = lax.broadcasted_iota(jnp.int32, (wide, 2 * WINDOW), 1)
    offset = key - jnp.where(lane >= WINDOW, lane - WINDOW, lane)
    near = (offset >= 0) & (offset <= 2 * WINDOW)
    side = lax.broadcasted_iota(jnp.int32, (1, 2 * WINDOW), 1)
    sink = jnp.where(side < WINDOW, sink_ref[0], sink_ref[1]) * LOG2E
    blocks = rows // WINDOW
    for n in range(blocks):
        k = ext[0:64, n * WINDOW : n * WINDOW + wide].T
        v = ext[64:128, n * WINDOW : n * WINDOW + wide]
        allowed = near
        if n == 0:
            allowed = allowed & ((key >= WINDOW) | jnp.logical_not(first_span))
        if n == blocks - 1:
            allowed = allowed & ((key < 2 * WINDOW) | jnp.logical_not(last_span))
        s = jnp.where(allowed, dot(k, q_ref[n]) * WINDOW_SCALE, -jnp.inf)
        top = jnp.maximum(jnp.max(s, axis=0, keepdims=True), sink)
        p = jnp.exp2(s - top)
        denom = jnp.sum(p, axis=0, keepdims=True) + jnp.exp2(sink - top)
        o = (dot(v, p.astype(BF16)) / denom).astype(BF16)
        out_ref[0:64, n * WINDOW : (n + 1) * WINDOW] = o[:, 0:WINDOW]
        out_ref[64:128, n * WINDOW : (n + 1) * WINDOW] = o[:, WINDOW:]


def windowed(span, q, kv, left, right, sink):
    smem = pl.BlockSpec(memory_space=pltpu.SMEM)
    vmem = pl.BlockSpec(memory_space=VMEM)
    rows = kv.shape[1]
    return pl.pallas_call(
        window_kernel,
        out_shape=jax.ShapeDtypeStruct((128, rows), BF16),
        in_specs=[smem, vmem, vmem, vmem, vmem, smem],
        out_specs=vmem,
        scratch_shapes=[VMEM((128, rows + 2 * WINDOW), BF16)],
        cost_estimate=pl.CostEstimate(
            flops=rows * 2 * 384 * 256, bytes_accessed=1 << 20, transcendentals=rows * 768
        ),
        compiler_params=params(),
        name="windowed",
    )(span, q, kv, left, right, sink)


def merge_kernel(place, keep_ref, got_ref, win_ref, wl_ref, ww_ref, *refs):
    own_refs, sib_ref, (mixed, lhs) = refs[:4], refs[4], refs[5:]
    sib_refs = [sib_ref.at[k] for k in range(4)]
    chip, core = place[0], place[2]
    for ref, half in ((keep_ref, core), (got_ref, 1 - core)):
        at = pl.ds(pl.multiple_of(half * TILE, TILE), TILE)
        mixed[0:HEAD, at] = ref[0]
        mixed[HEAD : 2 * HEAD, at] = ref[1]
    lhs[:, 0:128] = mixed[...].T
    lhs[:, 128:256] = win_ref[...].T
    rows = lhs[...]
    width = own_refs[0].shape[1]
    for outs, side in ((sib_refs, 1 - core), (own_refs, core)):
        for k in (2, 1, 3, 0):
            start = (2 * ((chip + k) % 4) + side) * width
            at = pl.ds(pl.multiple_of(start, width), width)
            both = jnp.concatenate([wl_ref[:, at], ww_ref[:, at]], axis=0)
            outs[k][...] = dot(rows, both).astype(BF16)


def merge(place, keep, got, win, out_latent, out_window):
    rows = win.shape[1]
    return pl.pallas_call(
        merge_kernel,
        out_shape=[jax.ShapeDtypeStruct((rows, 256), BF16)] * 4
        + [jax.ShapeDtypeStruct((4, rows, 256), BF16)],
        in_specs=[SMEM] + vmem(5),
        out_specs=vmem(5),
        scratch_shapes=[VMEM((128, rows), BF16), VMEM((rows, 256), BF16)],
        compiler_params=params(),
        cost_estimate=pl.CostEstimate(
            flops=2 * rows * 256 * 2048, bytes_accessed=4 << 20, transcendentals=0
        ),
        name="merge",
    )(place, keep, got, win, out_latent, out_window)


SWAP = [(0, 1), (1, 0)]


def shifted(value, axis, by):
    count = lax.axis_size(axis)
    return lax.ppermute(value, axis, [(i, (i + by) % count) for i in range(count)])


def other_core(value):
    return lax.ppermute(value, "c", SWAP)


def ring_step(value):
    count = lax.axis_size("z")
    up = [(2 * i, 2 * ((i + 1) % count)) for i in range(count)]
    down = [(2 * i + 1, 2 * ((i - 1) % count) + 1) for i in range(count)]
    return lax.ppermute(value, ("z", "c"), up + down)


def head_routes(turn):
    return [
        (2 * y + c, 2 * (2 * c + (y + turn) % 2) + y // 2) for y in range(4) for c in range(2)
    ]


def shards(
    inputs,
    norm_gain,
    latent_query,
    latent_down,
    rope_down,
    latent_gain,
    latent_up,
    window_query,
    window_key,
    window_value,
    sink_logit,
    out_latent,
    out_window,
):
    rows = inputs.shape[0]
    core = lax.axis_index("c")
    line = lax.axis_index("y")
    span = lax.axis_index(("z", "y"))
    spans = lax.axis_size(("z", "y"))
    slot = 2 * (line % 2) + core
    place = jnp.stack([lax.axis_index("x"), line, core, slot]).astype(jnp.int32)

    before = shifted(inputs, "x", 1)
    after = shifted(inputs, "x", -1)
    far_low = shifted(before[:TILE], "x", 1)
    far_high = shifted(after[TILE:], "x", -1)
    pieces = []
    for array in (inputs, before, after, far_low, far_high):
        pieces += [array, other_core(array)]
    powers = np.arange(0, HEAD, 2).astype(np.float64) / HEAD
    inverse = 1.0 / 10000.0**powers
    inverse = jnp.asarray(np.concatenate([inverse, inverse[::2]]), F32)
    positions = (span * rows + jnp.arange(rows)).astype(F32)
    angles = inverse[:, None] * positions[None, :]
    tables = jnp.cos(angles), jnp.sin(angles)
    *chunks, wq, wkv = project(
        place,
        (norm_gain.reshape(8, 1, 256), latent_gain[None], *tables),
        pieces,
        (
            latent_query.T,
            rope_down.T,
            window_key.T,
            window_value.T,
            window_query,
            latent_up,
            latent_down,
        ),
        rows,
    )
    arrived = []
    for r, chunk in enumerate(chunks):
        arrived.append(lax.ppermute(chunk, ("y", "c"), head_routes(r)))
    kept = jnp.stack([lax.dynamic_index_in_dim(a, core, 0, keepdims=False) for a in arrived])
    given = jnp.stack([lax.dynamic_index_in_dim(a, 1 - core, 0, keepdims=False) for a in arrived])
    mine = [kept, other_core(given)]
    left = lax.ppermute(
        wkv[:, rows - WINDOW :], ("z", "y"), [(i, i + 1) for i in range(spans - 1)]
    )
    right = lax.ppermute(
        wkv[:, :WINDOW], ("z", "y"), [(i + 1, i) for i in range(spans - 1)]
    )
    where = jnp.stack([span, spans]).astype(jnp.int32)
    win = windowed(where, wq, wkv, left, right, sink_logit)

    low = jnp.concatenate([c[:, 96:256] for c in mine])
    high = other_core(low)
    arriving = ring_step(low)
    state = attend(place, mine, [low, high], unroll=2)
    high = ring_step(high)
    low = arriving
    waiting = None
    for n in (1, 2, 3):
        arriving = ring_step(low)
        blocks = [low, other_core(low)]
        if waiting:
            state = attend(place, mine, waiting, state, unroll=2 if n == 2 else UNROLL)
        waiting = [high, other_core(high)]
        if n < 3:
            high = ring_step(high)
        state = attend(place, mine, blocks, state, unroll=2 if n == 1 else UNROLL)
        low = arriving
    blocks = [low, other_core(low)]
    state = attend(place, mine, waiting, state)
    (mixed,) = attend(place, mine, blocks, state, last=True)

    back = lax.all_to_all(mixed, "y", 0, 0, tiled=True)
    pairs = back.reshape(2, 2, HEAD, TILE)
    keep = lax.dynamic_index_in_dim(pairs, core, 0, keepdims=False)
    give = lax.dynamic_index_in_dim(pairs, 1 - core, 0, keepdims=False)
    sums = merge(place, keep, other_core(give), win, out_latent, out_window)
    siblings = other_core(sums[4])
    total = 0
    for k in (2, 1, 3, 0):
        both = sums[k].astype(F32) + siblings[k].astype(F32)
        if k:
            both = shifted(both.astype(BF16), "x", k).astype(F32)
        total = total + both
    return total.astype(BF16)


def solution(mesh):
    shape = (8, 4, 4, 2)
    torus = Mesh(mesh.devices.reshape(shape), ("z", "y", "x", "c"))
    sp, tp = ("z", "y"), ("x", "c")
    in_specs = (
        P(sp, tp),
        P(),
        P(None, tp),
        P(),
        P(),
        P(),
        P(None, tp),
        P(None, tp),
        P(None, tp),
        P(None, tp),
        P(tp),
        P(tp, None),
        P(tp, None),
    )
    return jax.shard_map(
        shards, mesh=torus, in_specs=in_specs, out_specs=P(sp, tp), check_vma=False
    )
```
